32 devices in a mesh: sp: 4 (over y, x), tp: 8 (over z, core).
Axes of the slice: x: 2, y: 2, z: 4, core: 2. Of those that a mesh axis runs over, the one named last changes fastest.
Arguments:
- pool_input: bfloat16 [16384, 512], P('sp', 'tp'), may hold values from -6 to 6
- gate_pre: bfloat16 [16384, 1024], P(('sp', 'tp')), may hold values from -8 to 8
- resid: bfloat16 [16384, 1024], P(('sp', 'tp')), may hold values from -6 to 6
- docs: int32 [16384], P('sp'), may hold values from 0 to 3, never falling along the last dimension, each value on 1 to 8192 neighbouring positions
- w_up: bfloat16 [512, 1024], replicated, may hold values from -0.25 to 0.25
- w_out: bfloat16 [1024, 1024], replicated, may hold values from -0.1875 to 0.1875
- g_ffn: float32 [1024], replicated, may hold values from 0.1 to 1.9
- w_gate: bfloat16 [4, 1024, 1024], P('sp'), may hold values from -0.5 to 0.5
- w_lift: bfloat16 [4, 1024, 1024], P('sp'), may hold values from -0.5 to 0.5
- w_down: bfloat16 [4, 1024, 1024], P('sp'), may hold values from -0.0390625 to 0.0390625
- routes: int32 [16384, 2], P(('sp', 'tp')), may hold values from 0 to 3, all different within a row; in each aligned block of 512 rows (0 to 511, 512 to 1023, ...) at most 320 rows name the same one
- route_weight: float32 [16384, 2], P(('sp', 'tp')), may hold values from 0.2 to 1
Outputs:
- layer_out: bfloat16 [16384, 1024], P(('sp', 'tp'))
The draws below stay inside these ranges and needn't reach their ends.
Inputs may be any that keep to these rules, and one draw needn't show every extreme that they name: `routes`: each row names 2 different experts; among the 512 rows of one device no expert is named more than 320 times. `docs`: document numbers never fall along the sequence.
All inputs are finite; a program needn't handle non-finite values.
Results may differ from the reference program's by a relative error of at most 0.0075.
Values may be sent and summed in bfloat16 or wider, within the bound.
No kernel may reach another device: no remote copies, remote signals or barrier semaphores. Data moves between devices by JAX's collectives and lax.ppermute only.
A program may use at most 128 MiB of HBM per device.

```python
import math
import jax
import jax.numpy as jnp
import numpy as np
from jax import lax

D = 1024
POOL_W = 512
HID = 1024
TOP = 2
RIM = 15
TOK_DEV = 4096
TOKENS = 16384
ROWS = 512
EXPERTS = 4
CAP = 320
N_SP = 4


def levels(stream_key, shape, shards, smallest, top_value):
    gain = 1.0
    for axis_at, parts in shards:
        steps = jax.random.uniform(jax.random.fold_in(jax.random.fold_in(stream_key, 6), axis_at), (parts,), jnp.float32, smallest / len(shards), top_value / len(shards))
        gain = gain * jnp.repeat(jnp.exp(steps), shape[axis_at] // parts).reshape((-1,) + (1,) * (len(shape) - 1 - axis_at))
    return gain


def length_profile(amount, total, limit, slope):
    portions = [(1 << 20) // math.isqrt(grade ** slope) + 1 for grade in range(2, amount + 1)]
    surplus, given = total - limit - (amount - 1), [1] * (amount - 1)
    while surplus > 0:
        candidates = [i for i in range(amount - 1) if given[i] < limit]
        mass, left = sum([portions[i] for i in candidates]), surplus
        for i in candidates:
            extra = min(limit - given[i], max(1, left * portions[i] // mass), surplus)
            given[i] = given[i] + extra
            surplus = surplus - extra
    return np.array([limit] + given)


def uneven_parts(own_key, number_of, total, reach, lean):
    if number_of == 2:
        one = jax.random.randint(own_key, (), max(1, total - reach), min(reach, total - 1) + 1)
        return jnp.stack([one, total - one])
    sizes = jnp.asarray(length_profile(number_of, total, reach, lean), jnp.int32)
    twos = (number_of - 1) // 2
    donor, taker = sizes[1:1 + 2 * twos:2], sizes[2:2 + 2 * twos:2]
    slack = jnp.minimum(donor - 1, reach - taker)
    moved = jax.random.randint(jax.random.fold_in(own_key, 1), (twos,), 0, 1 << 20) % (slack + 1)
    sizes = sizes.at[1:1 + 2 * twos:2].set(donor - moved).at[2:2 + 2 * twos:2].set(taker + moved)
    return sizes[jax.random.permutation(jax.random.fold_in(own_key, 2), number_of)]


def assign_block(stream_key, own, number, rows, count, top, limit, skew):
    order = jax.random.permutation(stream_key, count)
    packed, usual = shares(count, rows * top, limit, skew, True), shares(count, rows * top, limit, skew, False)
    places = jnp.arange(count)

    def named(lengths, turn):
        used = int((lengths > 0).sum())
        fixed = max(1, used // 4)
        passed = fixed + (places - fixed + turn * (used - fixed)) % max(1, count - fixed)
        return jnp.zeros((count,), jnp.int32).at[order[jnp.where(places < fixed, places, passed)]].set(jnp.asarray(lengths, jnp.int32))

    lengths = jnp.where(number % 4 == 0, named(packed, number // 4), named(usual, number - number // 4 - 1))
    mixed = jax.random.permutation(jax.random.fold_in(own, 3), count)
    source_of, sink = mixed[0:count // 2 * 2:2], mixed[1:count // 2 * 2:2]
    margin = jnp.minimum(lengths[source_of] - 1, limit - lengths[sink]) // 2
    margin = jnp.where((source_of == order[0]) | (sink == order[0]) | (lengths[sink] == 0), 0, jnp.maximum(margin, 0))
    passed = jax.random.randint(jax.random.fold_in(own, 4), (count // 2,), 0, 1 << 20) % (margin + 1)
    lengths = lengths.at[source_of].add(-passed).at[sink].add(passed)
    members = jnp.searchsorted(jnp.cumsum(lengths), jnp.arange(rows * top), side="right").astype(jnp.int32)
    grid = members.reshape(top, rows).T
    grid = grid[jax.random.permutation(jax.random.fold_in(own, 1), rows)]
    turn = jax.random.randint(jax.random.fold_in(own, 2), (rows, 1), 0, top)
    return jnp.take_along_axis(grid, (jnp.arange(top)[None, :] + turn) % top, axis=1)


def shares(number_of, total, reach, lean, full):
    loads = [(1 << 20) // math.isqrt(rank ** lean) + 1 for rank in range(1, number_of + 1)]
    largest = reach if full else min(reach, max(-(-total // number_of), total * loads[0] // sum(loads)))
    least = 1 if total - largest >= number_of - 1 else 0
    given, spare = [largest] + [least] * (number_of - 1), total - largest - least * (number_of - 1)
    while spare > 0:
        movable = [i for i in range(1, number_of) if given[i] < largest] or [i for i in range(1, number_of) if given[i] < reach]
        pool, budget = sum([loads[i] for i in movable]), spare
        for i in movable:
            extra = min(reach - given[i], max(1, budget * loads[i] // pool), spare)
            given[i] = given[i] + extra
            spare = spare - extra
    return np.array(given)


def bell_draw(stream_key, dims, deviation, bound, shards=(), held_as=jnp.bfloat16):
    drawn = jax.random.normal(stream_key, dims, jnp.float32) * deviation
    if len(shards) > 0:
        drawn = levels(stream_key, dims, shards, -0.22, 0.18) * drawn
    return jnp.clip(drawn, min=-bound, max=bound).astype(held_as)


def setup_inputs(seed: int = 0) -> dict:
    seeds = jax.random.split(jax.random.key(seed), 13)
    pool_input = bell_draw(seeds[0], (TOKENS, POOL_W), 1.0, 6.0, ((0, 4), (1, 8)))
    gate_pre = bell_draw(seeds[1], (TOKENS, D), 1.5, 8.0, ((0, 32),))
    resid = bell_draw(seeds[2], (TOKENS, D), 1.0, 6.0, ((0, 32),))
    docs = jnp.searchsorted(jnp.cumsum(uneven_parts(seeds[3], N_SP, TOKENS, 2 * TOK_DEV, 2)), jnp.arange(TOKENS), side="right").astype(jnp.int32)
    w_up = bell_draw(seeds[4], (POOL_W, D), POOL_W ** -0.5, 0.25)
    w_out = bell_draw(seeds[5], (D, D), D ** -0.5, 0.1875)
    g_ffn = jnp.clip(1.0 + 0.18 * jax.random.normal(seeds[6], (D,), jnp.float32), 0.1, 1.9)
    w_gate = bell_draw(seeds[7], (EXPERTS, D, HID), (D // 9) ** -0.5, 0.5, ((0, 4),))
    w_lift = bell_draw(seeds[8], (EXPERTS, D, HID), (D // 9) ** -0.5, 0.5, ((0, 4),))
    w_down = bell_draw(seeds[9], (EXPERTS, HID, D), (25 * HID) ** -0.5, 0.0390625, ((0, 4),))
    routes_keys = jax.random.split(jax.random.fold_in(seeds[10], 1), TOKENS // ROWS)
    routes_turns = jax.random.permutation(jax.random.fold_in(seeds[10], 3), TOKENS // ROWS)
    routes = jax.vmap(lambda own, number: assign_block(jax.random.fold_in(seeds[10], 2), own, number, ROWS, EXPERTS, TOP, CAP, 1))(routes_keys, routes_turns).reshape((TOKENS, TOP))
    route_weight = jnp.clip(0.2 + 0.8 * jax.random.uniform(seeds[11], (TOKENS, TOP), jnp.float32) ** levels(seeds[11], (TOKENS, TOP), ((0, 32),), -0.2, 0.2), 0.2, 1.0)
    return dict(pool_input=pool_input, gate_pre=gate_pre, resid=resid, docs=docs, w_up=w_up, w_out=w_out, g_ffn=g_ffn, w_gate=w_gate, w_lift=w_lift, w_down=w_down, routes=routes, route_weight=route_weight)


def pool_mixer(pool_input, docs):
    length = pool_input.shape[0]
    channels = pool_input.shape[1]
    group_size = POOL_W // 4
    channel_ids = lax.iota(jnp.int32, channels)
    window = jnp.power(2, channel_ids // group_size + 1)
    values = pool_input.astype(jnp.float32)
    padded = jnp.concatenate([jnp.zeros((RIM, channels), jnp.float32), values], axis=0)
    doc_padded = jnp.concatenate([jnp.full((RIM,), -1, jnp.int32), docs.astype(jnp.int32)], axis=0)
    running = jnp.zeros((length, channels), jnp.float32)
    counts = jnp.zeros((length, channels), jnp.float32)
    for offset in range(RIM + 1):
        shifted = padded[RIM - offset:RIM - offset + length]
        same_doc = (doc_padded[RIM - offset:RIM - offset + length] == docs).astype(jnp.float32)
        weight_mask = same_doc[:, None] * (offset < window).astype(jnp.float32)[None, :]
        running = running + weight_mask * shifted
        counts = counts + weight_mask
    return (running / counts - values).astype(jnp.bfloat16)

def reference(pool_input, gate_pre, resid, docs, w_up, w_out, g_ffn, w_gate, w_lift, w_down, routes, route_weight):
    pooled = pool_mixer(pool_input, docs)
    lifted = jnp.dot(pooled, w_up, preferred_element_type=jnp.float32)
    gated_rows = (jax.nn.sigmoid(gate_pre.astype(jnp.float32)) * lifted).astype(jnp.bfloat16)
    mixed_rows = (resid.astype(jnp.float32) + jnp.dot(gated_rows, w_out, preferred_element_type=jnp.float32)).astype(jnp.bfloat16)
    mixed_f = mixed_rows.astype(jnp.float32)
    normed = (mixed_f * lax.rsqrt(lax.optimization_barrier(jnp.mean(mixed_f * mixed_f, axis=-1, keepdims=True)) + 1e-06) * g_ffn).astype(jnp.bfloat16)
    gate_f = w_gate.astype(jnp.float32)
    lift_f = w_lift.astype(jnp.float32)
    down_f = w_down.astype(jnp.float32)
    blocks = TOKENS // ROWS
    model_dim = normed.shape[1]

    def one_block(inputs):
        block_rows, block_routes, block_weight, block_mixed = inputs
        flat_ids = block_routes.reshape(-1)
        onehot = (flat_ids[:, None] == lax.iota(jnp.int32, EXPERTS)[None, :]).astype(jnp.int32)
        slot_rank = lax.optimization_barrier(jnp.sum((jnp.cumsum(onehot, axis=0) - onehot) * onehot, axis=1))
        slot_index = flat_ids * CAP + slot_rank
        source = block_rows[lax.iota(jnp.int32, ROWS * TOP) // TOP]
        buffer = jnp.zeros((EXPERTS * CAP, model_dim), jnp.bfloat16).at[slot_index].set(source)
        buffer = buffer.reshape(EXPERTS, CAP, model_dim).astype(jnp.float32)
        gate_act = jnp.minimum(jnp.einsum('ekd,edh->ekh', buffer, gate_f), 7.0)
        lift = jnp.clip(jnp.einsum('ekd,edh->ekh', buffer, lift_f), -7.0, 7.0)
        act = ((lift + 1.0) * gate_act * jax.nn.sigmoid(1.702 * gate_act)).astype(jnp.bfloat16)
        expert_out = jnp.einsum('ekh,ehd->ekd', act.astype(jnp.float32), down_f).astype(jnp.bfloat16)
        returned = expert_out.reshape(EXPERTS * CAP, model_dim)[slot_index].astype(jnp.float32)
        returned = returned * block_weight.reshape(-1)[:, None]
        combined = lax.optimization_barrier(jnp.sum(returned.reshape(ROWS, TOP, model_dim), axis=1))
        return (block_mixed.astype(jnp.float32) + combined).astype(jnp.bfloat16)
    result = lax.map(one_block, (normed.reshape(blocks, ROWS, model_dim), routes.reshape(blocks, ROWS, TOP), route_weight.reshape(blocks, ROWS, TOP), mixed_rows.reshape(blocks, ROWS, model_dim)))
    return result.reshape(TOKENS, model_dim)
```

```python
import functools

import jax
import jax.numpy as jnp
from jax import lax
from jax.experimental import pallas as pl
from jax.experimental.pallas import tpu as pltpu
from jax.sharding import PartitionSpec as P

HALO = 16
LANES = 128
CHUNKS = 2
F32 = jnp.float32
BF16 = jnp.bfloat16
VMEM = pl.BlockSpec(memory_space=pltpu.VMEM)


def params(mib):
    return pltpu.CompilerParams(vmem_limit_bytes=mib * 1024 * 1024)


def dot(a, b):
    return jnp.dot(a, b, preferred_element_type=F32)


def mixer_kernel(
    x_ref, halo_ref, docs_ref, slot_ref, gate_ref, resid_ref, up_ref, out_ref, gain_ref,
    mixed_ref, packed_ref, pooled_ref, normed_ref,
):
    sources, per, rows = x_ref.shape
    wide = rows + LANES
    group = sources * per // 4
    each = group // per
    ids = docs_ref[...]
    same = [ids == pltpu.roll(ids, 1 << level, 1) for level in range(4)]
    keep = [s.astype(F32) for s in same]
    count = jnp.ones((1, wide), F32)
    for g in range(4):
        count = count + keep[g] * pltpu.roll(count, 1 << g, 1)
        scale = 1.0 / count[:, LANES:]
        own = x_ref[g * each : (g + 1) * each].astype(F32).reshape(group, rows)
        edge = jnp.concatenate(
            [halo_ref[g * each + i].astype(F32) for i in range(each)], axis=1
        )
        edge = jnp.concatenate([jnp.zeros((LANES - HALO, group), F32), edge], axis=0)
        run = jnp.concatenate([edge.T, own], axis=1)
        for level in range(g + 1):
            run = run + keep[level] * pltpu.roll(run, 1 << level, 1)
        pooled = run[:, LANES:] * scale - own
        pooled_ref[:, g * group : (g + 1) * group] = pooled.T.astype(BF16)
    step = min(256, rows)
    for r in range(0, rows, step):
        part = slice(r, r + step)
        lifted = dot(pooled_ref[part], up_ref[...])
        gated = (jax.nn.sigmoid(gate_ref[part].astype(F32)) * lifted).astype(BF16)
        mixed = (resid_ref[part].astype(F32) + dot(gated, out_ref[...])).astype(BF16)
        mixed_ref[part] = mixed
        wide_mixed = mixed.astype(F32)
        norm = lax.rsqrt(jnp.mean(wide_mixed * wide_mixed, axis=-1, keepdims=True) + 1e-06)
        normed_ref[part] = (wide_mixed * norm * gain_ref[...]).astype(BF16)
    blocks, size, _ = packed_ref.shape
    for b in range(blocks):
        places = b * size + lax.broadcasted_iota(jnp.int32, (size, rows), 0)
        hit = jnp.zeros((size, rows), F32)
        for k in range(slot_ref.shape[0]):
            hit = jnp.where(places == slot_ref[k : k + 1, :], 1.0, hit)
        packed_ref[b] = dot(hit.astype(BF16), normed_ref[...]).astype(BF16)


def mixer(x, halo, docs, slots, gate_pre, resid, w_up, w_out, gain, blocks, size):
    rows, dim = resid.shape
    return pl.pallas_call(
        mixer_kernel,
        out_shape=(
            jax.ShapeDtypeStruct((rows, dim), BF16),
            jax.ShapeDtypeStruct((blocks, size, dim), BF16),
        ),
        in_specs=[VMEM] * 9,
        out_specs=(VMEM, VMEM),
        scratch_shapes=[
            pltpu.VMEM((rows, x.shape[0] * x.shape[1]), BF16),
            pltpu.VMEM((rows, dim), BF16),
        ],
        compiler_params=params(48),
        name="mixer",
    )(x, halo, docs, slots, gate_pre, resid, w_up, w_out, gain)


def expert_kernel(count, *refs):
    parts, (gate_ref, lift_ref, down_ref), outs = (
        refs[:count],
        refs[count : count + 3],
        refs[count + 3 : 2 * count + 3],
    )
    act_ref = refs[-1]
    rows = jnp.concatenate([p[...] for p in parts], axis=0) if count > 1 else parts[0][...]
    hidden = gate_ref.shape[1]
    step = min(256, hidden)
    for h in range(0, hidden, step):
        part = slice(h, h + step)
        gate = jnp.minimum(dot(rows, gate_ref[:, part]), 7.0)
        lift = jnp.clip(dot(rows, lift_ref[:, part]), -7.0, 7.0)
        act_ref[:, part] = ((lift + 1.0) * gate * jax.nn.sigmoid(1.702 * gate)).astype(BF16)
    size = parts[0].shape[0]
    for h in range(0, down_ref.shape[1], step):
        part = slice(h, h + step)
        done = dot(act_ref[...], down_ref[:, part]).astype(BF16)
        for i, out in enumerate(outs):
            out[:, part] = done[i * size : (i + 1) * size]


def expert(parts, w_gate, w_lift, w_down):
    count, (size, dim) = len(parts), parts[0].shape
    out = jax.ShapeDtypeStruct((size, w_down.shape[1]), BF16)
    return pl.pallas_call(
        functools.partial(expert_kernel, count),
        out_shape=(out,) * count,
        in_specs=[VMEM] * (count + 3),
        out_specs=(VMEM,) * count,
        scratch_shapes=[pltpu.VMEM((count * size, w_gate.shape[1]), BF16)],
        compiler_params=params(32),
        name="expert",
    )(*parts, w_gate, w_lift, w_down)


def combine_kernel(starts, slot_ref, weight_ref, mixed_ref, *refs):
    parts, out_ref = refs[:-1], refs[-1]
    rows, dim = mixed_ref.shape
    step = min(256, rows)
    for r in range(0, rows, step):
        span = slice(r, r + step)
        total = mixed_ref[span].astype(F32)
        for start, part in zip(starts, parts):
            size = part.shape[0]
            places = start + lax.broadcasted_iota(jnp.int32, (step, size), 1)
            hit = jnp.zeros((step, size), F32)
            for k in range(slot_ref.shape[1]):
                hit = jnp.where(
                    places == slot_ref[span, k : k + 1], weight_ref[span, k : k + 1], hit
                )
            total = total + dot(hit.astype(BF16), part[...])
        out_ref[span] = total.astype(BF16)


def combine(starts, slots, weights, mixed, parts):
    return pl.pallas_call(
        functools.partial(combine_kernel, tuple(starts)),
        out_shape=jax.ShapeDtypeStruct(mixed.shape, BF16),
        in_specs=[VMEM] * (3 + len(parts)),
        out_specs=VMEM,
        compiler_params=params(32),
        name="combine",
    )(slots, weights, mixed, *parts)


def on_device(
    pool_input,
    gate_pre,
    resid,
    docs,
    w_up,
    w_out,
    g_ffn,
    w_gate,
    w_lift,
    w_down,
    routes,
    route_weight,
):
    tok_dev, channels = pool_input.shape
    rows, dim = resid.shape
    tp_count, sp_count = lax.axis_size("tp"), lax.axis_size("sp")
    sp_at, tp_at = lax.axis_index("sp"), lax.axis_index("tp")
    top = routes.shape[1]
    experts = sp_count * w_gate.shape[0]
    cap = max(2, 5 * rows * top // (4 * experts))

    by_channel = pool_input.T.reshape(channels, tp_count, rows).transpose(1, 0, 2)
    x = lax.all_to_all(by_channel, "tp", split_axis=0, concat_axis=0, tiled=True)

    tails = pool_input.reshape(tp_count, rows, channels)[:, rows - HALO :]
    tail_docs = jnp.pad(docs[tok_dev - HALO :].astype(BF16), (0, channels - HALO))
    edge = lax.ppermute(
        jnp.concatenate([tails[-1], tail_docs[None]], axis=0),
        "sp",
        [(i, i + 1) for i in range(sp_count - 1)],
    )
    halo_out = jnp.concatenate([edge[None, :HALO], tails[:-1]], axis=0)
    halo = lax.all_to_all(halo_out, "tp", split_axis=0, concat_axis=0, tiled=True)
    before = jnp.where(sp_at == 0, -1, edge[HALO, :HALO].astype(jnp.int32))
    all_docs = jnp.concatenate([jnp.full((LANES - HALO,), -2, jnp.int32), before, docs])
    near_docs = lax.dynamic_slice(all_docs, (tp_at * rows,), (LANES + rows,))[None]

    picks = routes.T
    ids = lax.iota(jnp.int32, experts)
    named = picks[:, None, :] == ids[None, :, None]
    earlier = (lax.iota(jnp.int32, rows)[:, None] < lax.iota(jnp.int32, rows)[None, :]).astype(BF16)
    rank = dot(jnp.any(named, axis=0).astype(BF16), earlier).astype(jnp.int32)
    home = ((ids ^ sp_at) * cap)[:, None]
    slots = jnp.sum(jnp.where(named, (rank + home)[None], 0), axis=1)

    mixed, packed = mixer(
        x, halo, near_docs, slots, gate_pre, resid, w_up, w_out, g_ffn[None], sp_count, cap
    )

    weights = (w_gate[0], w_lift[0], w_down[0])
    chunks = CHUNKS if cap % (16 * CHUNKS) == 0 else 1
    size = cap // chunks

    def swap(value, offset):
        return lax.ppermute(value, "sp", [(i, i ^ offset) for i in range(sp_count)])

    starts, parts = [0], list(expert([packed[0]], *weights))
    for c in range(chunks):
        arrived = [
            swap(packed[o, c * size : (c + 1) * size], o) for o in range(1, sp_count)
        ]
        done = expert(arrived, *weights)
        parts += [swap(d, o) for d, o in zip(done, range(1, sp_count))]
        starts += [o * cap + c * size for o in range(1, sp_count)]
    return combine(starts, slots.T, route_weight, mixed, parts)


def solution(mesh):
    in_specs = (
        P("sp", "tp"),
        P(("sp", "tp"), None),
        P(("sp", "tp"), None),
        P("sp"),
        P(),
        P(),
        P(),
        P("sp", None, None),
        P("sp", None, None),
        P("sp", None, None),
        P(("sp", "tp"), None),
        P(("sp", "tp"), None),
    )
    out_specs = P(("sp", "tp"), None)
    return jax.shard_map(
        on_device, mesh=mesh, in_specs=in_specs, out_specs=out_specs, check_vma=False
    )
```
